512 devices in a mesh: fs: 16 (over y, x), tp: 32 (over z, core).
Axes of the slice: x: 4, y: 4, z: 16, core: 2. Of those that a mesh axis runs over, the one named last changes fastest.
Arguments:
- saved_inputs: bfloat16 [10752, 4096], P('fs', 'tp'), may hold values from -6 to 6
- proj_cotangent: bfloat16 [10752, 4096], P('fs', 'tp'), may hold values from -0.057861328 to 0.057861328
- saved_hidden: bfloat16 [10752, 4096], P('fs', 'tp'), may hold values from -6 to 6
- out_cotangent: bfloat16 [10752, 4096], P('fs', 'tp'), may hold values from -0.057861328 to 0.057861328
- factors: bfloat16 [2, 4096, 128], replicated, may hold values from -0.46875 to 0.46875
- w_proj: float32 [4096, 4096], P('fs', 'tp'), may hold values from -0.09375 to 0.09375
- w_out: float32 [4096, 4096], P('tp', 'fs'), may hold values from -0.09375 to 0.09375
- moment_first: float32 [2, 128, 4096], P(None, None, 'tp'), may hold values from -1.8 to 1.8
- moment_second: float32 [2, 128, 4096], P(None, None, 'tp'), may hold values from 0.05 to 1
Outputs:
- proj_next: float32 [4096, 4096], P('fs', 'tp')
- out_next: float32 [4096, 4096], P('tp', 'fs')
- proj_copy: bfloat16 [4096, 4096], P(None, 'tp')
- out_copy: bfloat16 [4096, 4096], P('tp')
- first_next: float32 [2, 128, 4096], P(None, None, 'tp')
- second_next: float32 [2, 128, 4096], P(None, None, 'tp')
The draws below stay inside these ranges and needn't reach their ends.
All inputs are finite; a program needn't handle non-finite values.
Results may differ from the reference program's by a relative error of at most 0.001.
Values may be sent and summed in bfloat16 or wider, within the bound.
No kernel may reach another device: no remote copies, remote signals or barrier semaphores. Data moves between devices by JAX's collectives and lax.ppermute only.
A program may use at most 64 MiB of HBM per device.

```python
import math
import jax
import jax.numpy as jnp
from jax import lax

D = 4096
E = 4096
RANK = 128
TOKENS = 10752


def draw_factors(key, part):
    base_key, rough_key = jax.random.split(jax.random.fold_in(key, 11))
    position = jnp.arange(D, dtype=jnp.float32) / max(D - 1, 1)
    rough = jnp.exp(jax.random.uniform(rough_key, (2, D, 1), jnp.float32, 0.0, math.log(4.0)))
    base = jnp.clip(jax.random.normal(base_key, (2, D, RANK), jnp.float32), -4.0, 4.0)
    rising = jnp.exp(position * math.log(3.0))
    values = base * rough * rising[None, :, None] * (0.5 / math.sqrt(D))
    return values.astype(jnp.bfloat16)


def block_levels(key, dims, pieces, smallest, high):
    def one(axis_at, parts):
        draws = jax.random.uniform(jax.random.fold_in(jax.random.fold_in(key, 6), axis_at), (parts,), jnp.float32, smallest / len(pieces), high / len(pieces))
        return jnp.repeat(jnp.exp(draws), dims[axis_at] // parts).reshape((-1,) + (1,) * (len(dims) - axis_at - 1))

    factor_of = one(*pieces[0])
    for cut in pieces[1:]:
        factor_of = factor_of * one(*cut)
    return factor_of


def scatter_about(stream_key, dims, width, limit, pieces=(), kind=jnp.bfloat16):
    factor_of = block_levels(stream_key, dims, pieces, -0.22, 0.18) if pieces else 1.0
    entries = jax.random.normal(stream_key, dims, jnp.float32) * width * factor_of
    return jnp.minimum(jnp.maximum(entries, -limit), limit).astype(kind)


def setup_inputs(seed: int = 0) -> dict:
    keys = jax.random.split(jax.random.key(seed), 10)
    saved_inputs = scatter_about(keys[0], (TOKENS, D), 1.0, 6.0, ((0, 16), (1, 32)))
    proj_cotangent = scatter_about(keys[1], (TOKENS, E), (TOKENS ** -0.5), 0.057861328, ((0, 16), (1, 32)))
    saved_hidden = scatter_about(keys[2], (TOKENS, E), 1.0, 6.0, ((0, 16), (1, 32)))
    out_cotangent = scatter_about(keys[3], (TOKENS, D), (TOKENS ** -0.5), 0.057861328, ((0, 16), (1, 32)))
    factors = draw_factors(jax.random.fold_in(keys[9], 71), 0)
    w_proj = scatter_about(keys[5], (D, E), D ** -0.5, 0.09375, ((0, 16), (1, 32)), jnp.float32)
    w_out = scatter_about(keys[6], (E, D), E ** -0.5, 0.09375, ((0, 32), (1, 16)), jnp.float32)
    moment_first = scatter_about(keys[7], (2, RANK, E), 0.3, 1.8, ((2, 32),), jnp.float32)
    moment_second = jnp.clip(jnp.exp(math.log(1.0) - 2.9957323 * jax.random.uniform(keys[8], (2, RANK, E), jnp.float32) ** block_levels(keys[8], (2, RANK, E), ((2, 32),), -0.2, 0.2)), 0.05, 1.0)
    return {"saved_inputs": saved_inputs, "proj_cotangent": proj_cotangent, "saved_hidden": saved_hidden, "out_cotangent": out_cotangent, "factors": factors, "w_proj": w_proj, "w_out": w_out, "moment_first": moment_first, "moment_second": moment_second}


beta_first = 0.9
beta_second = 0.95
learn_rate = 0.02
epsilon = 1e-06

def reference(saved_inputs, proj_cotangent, saved_hidden, out_cotangent, factors, w_proj, w_out, moment_first, moment_second):
    highest = lax.Precision.HIGHEST
    factor_full = factors.astype(jnp.float32)
    grad_proj = jnp.dot(saved_inputs.T, proj_cotangent, preferred_element_type=jnp.float32)
    grad_out_t = jnp.dot(out_cotangent.T, saved_hidden, preferred_element_type=jnp.float32)
    small_grads = jnp.stack([jnp.dot(factor_full[0].T, grad_proj, precision=highest), jnp.dot(factor_full[1].T, grad_out_t, precision=highest)])
    first_next = beta_first * moment_first + (1.0 - beta_first) * small_grads
    second_next = beta_second * moment_second + (1.0 - beta_second) * small_grads * small_grads
    direction = first_next / (jnp.sqrt(second_next) + epsilon)
    update_full = jnp.einsum('kdr,kre->kde', factor_full, direction, precision=highest)
    norm_scale = lax.rsqrt(lax.optimization_barrier(jnp.mean(update_full * update_full, axis=(1, 2))) + epsilon)
    stepped = update_full * norm_scale[:, None, None]
    proj_next = w_proj - learn_rate * stepped[0]
    out_next = w_out - learn_rate * stepped[1].T
    return (proj_next, out_next, proj_next.astype(jnp.bfloat16), out_next.astype(jnp.bfloat16), first_next, second_next)
```

```python
import jax
import jax.numpy as jnp
from jax import lax
from jax.sharding import Mesh
from jax.sharding import PartitionSpec as P

FS = ("fs_0", "fs_1")
TP = ("tp_0", "tp_1")


beta_first = 0.9
beta_second = 0.95
learn_rate = 0.02
epsilon = 1e-06
HIGHEST = lax.Precision.HIGHEST


def exchange(x, axis):
    return lax.all_to_all(x, axis, 0, 0, tiled=True)


def sent_to_all(x, axis):
    return exchange(jnp.broadcast_to(x[None], (lax.axis_size(axis), *x.shape)), axis)


def three_parts(x):
    high = lax.reduce_precision(x, 8, 7)
    rest = x - high
    middle = lax.reduce_precision(rest, 8, 7)
    low = rest - middle
    return [p.astype(jnp.bfloat16) for p in (high, middle, low)]


def dot_with_parts(parts, dims, other):
    return sum(
        lax.dot_general(other, p, (dims, ((), ())), preferred_element_type=jnp.float32)
        for p in parts[::-1]
    )


def body(
    saved_inputs,
    proj_cotangent,
    saved_hidden,
    out_cotangent,
    factors,
    w_proj,
    w_out,
    moment_first,
    moment_second,
):
    fs_count = lax.axis_size(FS)
    tp_count = lax.axis_size(TP)
    z_count = lax.axis_size("tp_0")
    core = lax.axis_index("tp_1")
    d_model, rank = factors.shape[1:]
    tokens, feats = saved_inputs.shape
    hidden = proj_cotangent.shape[1]
    fs_rows = d_model // fs_count

    tiles = fs_rows // hidden
    w_out_tiles = jnp.moveaxis(w_out.reshape(hidden, tiles, hidden), 1, 0)
    own_w = jnp.concatenate([w_proj, w_out_tiles.reshape(fs_rows, hidden)])
    all_w = lax.all_gather(own_w, FS, axis=0, tiled=False)

    chunk = -(-tokens // (16 * z_count)) * 16
    spare = chunk * z_count - tokens

    def in_chunks(x):
        return jnp.pad(x, ((0, spare), (0, 0))).reshape(z_count, chunk, feats)

    sends = jnp.stack([in_chunks(saved_inputs), in_chunks(out_cotangent)], axis=1)
    rows = exchange(sends.reshape(tp_count, chunk, feats), TP)
    mine = lax.dynamic_index_in_dim(factors, core, 0, keepdims=False)
    mine = mine.reshape(tp_count, feats, rank)
    y_chunk = jnp.sum(
        lax.dot_general(
            rows, mine, (((2,), (1,)), ((0,), (0,))), preferred_element_type=jnp.float32
        ),
        axis=0,
    )
    y = lax.all_gather(y_chunk, TP, axis=0, tiled=False).reshape(z_count, 2, chunk, rank)

    def over_tokens(k, right):
        left = y[:, k].reshape(z_count * chunk, rank)[:tokens]
        return lax.dot_general(
            left,
            right.astype(jnp.float32),
            (((0,), (0,)), ((), ())),
            preferred_element_type=jnp.float32,
            precision=HIGHEST,
        )

    partial = jnp.concatenate([over_tokens(0, proj_cotangent), over_tokens(1, saved_hidden)])
    own_sum = jnp.sum(exchange(partial.reshape(fs_count, -1, hidden), FS), axis=0)
    small_grads = sent_to_all(own_sum, FS).reshape(2, rank, hidden)

    first_next = beta_first * moment_first + (1.0 - beta_first) * small_grads
    second_next = beta_second * moment_second + (1.0 - beta_second) * small_grads * small_grads
    direction = first_next / (jnp.sqrt(second_next) + epsilon)

    gram = lax.dot_general(
        factors, factors, (((1,), (1,)), ((0,), (0,))), preferred_element_type=jnp.float32
    )
    spread = jnp.einsum("krs,kse->kre", gram, direction, precision=HIGHEST)
    squares = jnp.maximum(jnp.sum(direction * spread, axis=(1, 2)), 0.0)
    totals = jnp.sum(sent_to_all(squares[None], TP), axis=(0, 1))
    norm_scale = lax.rsqrt(totals / (d_model * hidden * tp_count) + epsilon)
    step = learn_rate * norm_scale

    update_0 = dot_with_parts(three_parts(direction[0]), ((1,), (0,)), factors[0])
    update_1 = sum(
        lax.dot_general(
            p, factors[1], (((0,), (1,)), ((), ())), preferred_element_type=jnp.float32
        )
        for p in three_parts(direction[1])[::-1]
    )
    update_0, update_1 = lax.optimization_barrier((update_0, update_1))

    start = lax.axis_index(FS) * fs_rows
    own_0 = lax.dynamic_slice_in_dim(update_0, start, fs_rows, 0)
    own_1 = lax.dynamic_slice_in_dim(update_1, start, fs_rows, 1)
    proj_next = w_proj - step[0] * own_0
    out_next = w_out - step[1] * own_1
    all_proj = all_w[:, :fs_rows].reshape(d_model, hidden)
    proj_copy = (all_proj - step[0] * update_0).astype(jnp.bfloat16)
    all_out = all_w[:, fs_rows:].reshape(d_model // hidden, hidden, hidden)
    all_out = jnp.moveaxis(all_out, 0, 1).reshape(hidden, d_model)
    out_copy = (all_out - step[1] * update_1).astype(jnp.bfloat16)
    return (proj_next, out_next, proj_copy, out_copy, first_next, second_next)


def solution(mesh):
    torus = Mesh(mesh.devices.reshape(4, 4, 16, 2), ("fs_0", "fs_1", "tp_0", "tp_1"))
    return jax.shard_map(
        body,
        mesh=torus,
        in_specs=(
            P(FS, TP),
            P(FS, TP),
            P(FS, TP),
            P(FS, TP),
            P(),
            P(FS, TP),
            P(TP, FS),
            P(None, None, TP),
            P(None, None, TP),
        ),
        out_specs=(
            P(FS, TP),
            P(TP, FS),
            P(None, TP),
            P(TP, None),
            P(None, None, TP),
            P(None, None, TP),
        ),
        check_vma=False,
    )
```
